32 devices in a mesh: fs: 8 (over z, x), tp: 4 (over y, core).
Axes of the slice: x: 2, y: 2, z: 4, core: 2. Of those that a mesh axis runs over, the one named last changes fastest.
Arguments:
- inputs: bfloat16 [8192, 4096], P('fs'), may hold values from -8 to 8
- value_cot: bfloat16 [8192, 2048], P('fs', 'tp'), may hold values from -0.015625 to 0.015625
- gate_cot: bfloat16 [8192, 2048], P('fs', 'tp'), may hold values from -0.015625 to 0.015625
- out_cot: bfloat16 [8192, 4096], P('fs'), may hold values from -0.0234375 to 0.0234375
- conv_output: bfloat16 [8192, 2048], P('fs', 'tp'), may hold values from -6 to 6
- factors: bfloat16 [3, 4096, 256], P(None, 'fs'), may hold values from -0.375 to 0.375
- value_weight: float32 [4096, 2048], P('fs', 'tp'), may hold values from -0.09375 to 0.09375
- gate_weight: float32 [4096, 2048], P('fs', 'tp'), may hold values from -0.09375 to 0.09375
- out_weight: float32 [2048, 4096], P('tp', 'fs'), may hold values from -0.125 to 0.125
- first_moment: float32 [3, 256, 2048], P(None, 'fs', 'tp'), may hold values from -7.2 to 7.2
- second_moment: float32 [3, 256, 2048], P(None, 'fs', 'tp'), may hold values from 0.005 to 0.05
Outputs:
- new_first: float32 [3, 256, 2048], P(None, 'fs', 'tp')
- new_second: float32 [3, 256, 2048], P(None, 'fs', 'tp')
- value_update: float32 [4096, 2048], P('fs', 'tp')
- gate_update: float32 [4096, 2048], P('fs', 'tp')
- out_update: float32 [2048, 4096], P('tp', 'fs')
- value_copy: bfloat16 [4096, 2048], P(None, 'tp')
- gate_copy: bfloat16 [4096, 2048], P(None, 'tp')
- out_copy: bfloat16 [2048, 4096], P('tp')
The draws below stay inside these ranges and needn't reach their ends.
All inputs are finite; a program needn't handle non-finite values.
Results may differ from the reference program's by a relative error of at most 0.001.
Values may be sent and summed in bfloat16 or wider, within the bound.
A program may use at most 128 MiB of HBM per device.

```python
import math
import jax
import jax.numpy as jnp
from jax import lax

D = 4096
C = 2048
RANK = 256
TOKENS = 8192


def draw_first_moment(key, part):
    key_one, key_two = jax.random.split(jax.random.fold_in(key, 11), 2)
    row_rise = jnp.arange(RANK, dtype=jnp.float32) / max(RANK - 1, 1)
    col_rise = jnp.arange(C, dtype=jnp.float32) / max(C - 1, 1)
    rise_table = jnp.exp(jnp.log(3.0) * row_rise)[:, None] * jnp.exp(jnp.log(3.0) * col_rise)[None, :]
    roughness = jnp.exp(jax.random.uniform(key_two, (3, RANK, C), jnp.float32, 0.0, jnp.log(2.0)))
    base_draw = jnp.clip(jax.random.normal(key_one, (3, RANK, C), jnp.float32), -4.0, 4.0)
    return (0.1 * base_draw * rise_table[None, :, :] * roughness).astype(jnp.float32)


def spiked(result, rng, source, target, blocks, factor):
    owner, partner = [(jnp.arange(result.shape[axis_at]) // (result.shape[axis_at] // blocks)).reshape([-1 if axis == axis_at else 1 for axis in range(result.ndim)]) for axis_at in (source, target)]
    chosen = jax.random.permutation(rng, blocks)[partner]
    strong = (owner == chosen) | (owner == (partner + blocks // 2) % blocks)
    return jnp.where(strong, factor * result, result)


def block_levels(stream_key, extent, cuts, least, largest):
    factor_of = 1.0
    for dim, parts in cuts:
        draws = jax.random.uniform(jax.random.fold_in(jax.random.fold_in(stream_key, 6), dim), (parts,), jnp.float32, least / len(cuts), largest / len(cuts))
        factor_of = factor_of * jnp.repeat(jnp.exp(draws), extent[dim] // parts).reshape((-1,) + (1,) * (len(extent) - 1 - dim))
    return factor_of


def centred(own_key, dims, deviation, bound, cuts=(), held_as=jnp.bfloat16):
    result = deviation * jax.random.normal(own_key, dims, jnp.float32)
    if cuts:
        result = result * block_levels(own_key, dims, cuts, -0.22, 0.18)
    return jnp.clip(result, -bound, bound).astype(held_as)


def gaussian_with(key, extent, width, limit, pieces, heavy, kind=jnp.bfloat16):
    array = width * jax.random.normal(key, extent, jnp.float32)
    if pieces:
        array = array * block_levels(key, extent, pieces, -0.22, 0.18)
    return jnp.clip(spiked(array, jax.random.fold_in(key, 3), *heavy), -limit, limit).astype(kind)


def setup_inputs(seed: int = 0) -> dict:
    keys = jax.random.split(jax.random.key(seed), 12)
    inputs = gaussian_with(keys[0], (TOKENS, D), 1.0, 8.0, ((0, 8),), (0, 1, 8, 2.0))
    value_cot = centred(keys[1], (TOKENS, C), (RANK ** 0.5 * (D * TOKENS) ** -0.5), 0.015625, ((0, 8), (1, 4)))
    gate_cot = centred(keys[2], (TOKENS, C), (RANK ** 0.5 * (D * TOKENS) ** -0.5), 0.015625, ((0, 8), (1, 4)))
    out_cot = gaussian_with(keys[3], (TOKENS, D), (RANK ** 0.5 * (D * TOKENS) ** -0.5), 0.0234375, ((0, 8),), (0, 1, 8, 2.0))
    conv_output = centred(keys[4], (TOKENS, C), 1.0, 6.0, ((0, 8), (1, 4)))
    factors = centred(keys[5], (3, D, RANK), RANK ** -0.5, 0.375, ((1, 8),))
    value_weight = centred(keys[6], (D, C), D ** -0.5, 0.09375, ((0, 8), (1, 4)), jnp.float32)
    gate_weight = centred(keys[7], (D, C), D ** -0.5, 0.09375, ((0, 8), (1, 4)), jnp.float32)
    out_weight = centred(keys[8], (C, D), C ** -0.5, 0.125, ((0, 4), (1, 8)), jnp.float32)
    first_moment = draw_first_moment(jax.random.fold_in(keys[11], 71), 0)
    second_moment = jnp.clip(jnp.exp(math.log(0.05) - 2.3025851 * jax.random.uniform(keys[10], (3, RANK, C), jnp.float32) ** block_levels(keys[10], (3, RANK, C), ((1, 8), (2, 4)), -0.2, 0.2)), 0.005, 0.05)
    return dict(inputs=inputs, value_cot=value_cot, gate_cot=gate_cot, out_cot=out_cot, conv_output=conv_output, factors=factors, value_weight=value_weight, gate_weight=gate_weight, out_weight=out_weight, first_moment=first_moment, second_moment=second_moment)


FIRST_DECAY = 0.9
SECOND_DECAY = 0.95
DIVISOR_EPS = 1e-08
SQUARE_EPS = 1e-06
LEARN_RATE = 0.01

def project_side(source, factor, target):
    left_proj = jnp.dot(source.astype(jnp.float32), factor.astype(jnp.float32), precision=lax.Precision.HIGHEST)
    return jnp.dot(left_proj.T, target.astype(jnp.float32), precision=lax.Precision.HIGHEST)

def reference(inputs, value_cot, gate_cot, out_cot, conv_output, factors, value_weight, gate_weight, out_weight, first_moment, second_moment):
    projected = jnp.stack([project_side(inputs, factors[0], value_cot), project_side(inputs, factors[1], gate_cot), project_side(out_cot, factors[2], conv_output)])
    new_first = FIRST_DECAY * first_moment + (1.0 - FIRST_DECAY) * projected
    new_second = SECOND_DECAY * second_moment + (1.0 - SECOND_DECAY) * projected * projected
    direction = new_first / (jnp.sqrt(new_second) + DIVISOR_EPS)
    total = jnp.sum(direction * direction)
    norm_scale = lax.rsqrt(total / (3 * RANK * C) + SQUARE_EPS)
    float_factors = factors.astype(jnp.float32)
    value_update = norm_scale * jnp.dot(float_factors[0], direction[0], precision=lax.Precision.HIGHEST)
    gate_update = norm_scale * jnp.dot(float_factors[1], direction[1], precision=lax.Precision.HIGHEST)
    out_update = (norm_scale * jnp.dot(float_factors[2], direction[2], precision=lax.Precision.HIGHEST)).T
    value_copy = (value_weight - LEARN_RATE * value_update).astype(jnp.bfloat16)
    gate_copy = (gate_weight - LEARN_RATE * gate_update).astype(jnp.bfloat16)
    out_copy = (out_weight - LEARN_RATE * out_update).astype(jnp.bfloat16)
    return (new_first, new_second, value_update, gate_update, out_update, value_copy, gate_copy, out_copy)
```

```python
import functools

import jax
import jax.numpy as jnp
from jax import lax
from jax.experimental import pallas as pl
from jax.experimental.pallas import tpu as pltpu
from jax.sharding import PartitionSpec as P

FIRST_DECAY = 0.9
SECOND_DECAY = 0.95
DIVISOR_EPS = 1e-08
SQUARE_EPS = 1e-06
LEARN_RATE = 0.01
MESH = pl.DeviceIdType.MESH
F32 = jnp.float32
BF16 = jnp.bfloat16


def high_low(values):
    upper = values.astype(BF16)
    lower = (values - upper.astype(F32)).astype(BF16)
    return upper, lower


def others(coord, size, dist):
    if dist == 0:
        return [(coord, 0, None)]
    if size == 2:
        return [(1 - coord, None, None)]
    return [(coord - dist, -1, coord >= dist), (coord + dist, 1, coord + dist < size)]


def both(*preds):
    preds = [p for p in preds if p is not None]
    if not preds:
        return None
    return functools.reduce(jnp.logical_and, preds)


def run_if(pred, fn):
    if pred is None:
        fn()
    else:
        pl.when(pred)(fn)


def kernel(
    nz, nx, tp,
    x_hbm, oc_hbm, vc_hbm, gc_hbm, co_hbm, f_hbm, w0_hbm, w1_hbm, w2_hbm, m1_ref, m2_ref,
    nf_ref, ns_ref, u0_hbm, u1_hbm, u2_hbm, c0_hbm, c1_hbm, c2_hbm,
    x_v, oc_v, cots, fg, wts, acc, part, rx, rz, q, dg, dh, dl, upd, upd_t, own01, own2, ss,
    in_sem, loc_sem, f_recv, f_send, y_recv, y_send, p_recv, p_send,
    rx_recv, rx_send, rz_recv, rz_send, d_recv, d_send, s_recv, s_send, c_recv, c_send,
):
    me = lax.axis_index("fs")
    t = lax.axis_index("tp")
    z = lax.div(me, nx)
    x = lax.rem(me, nx)
    n = nz * nx
    core = lax.rem(t, 2)
    row = lax.rem(lax.div(t, 2), 2)
    mate = t + 1 - 2 * core
    beside = t + 2 - 4 * row
    block = f_hbm.shape[1]
    rank = f_hbm.shape[2]
    rows = m1_ref.shape[1]
    width = m1_ref.shape[2]
    tokens = x_hbm.shape[0]
    pending = []

    def remote(src, dst, ssem, rsem, where):
        copy = pltpu.make_async_remote_copy(
            src_ref=src, dst_ref=dst, send_sem=ssem, recv_sem=rsem,
            device_id=where, device_id_type=MESH,
        )
        return copy

    def send(src, dst, ssem, rsem, where, pred, outer):
        copy = remote(src, dst, ssem, rsem, where)
        pred = both(pred, outer)
        run_if(pred, copy.start)
        pending.append((pred, copy))

    def drain():
        for pred, copy in pending:
            run_if(pred, copy.wait_send)
        pending.clear()

    loads = [
        pltpu.make_async_copy(f_hbm, fg.at[me], in_sem.at[0]),
        pltpu.make_async_copy(x_hbm, x_v, in_sem.at[1]),
        pltpu.make_async_copy(oc_hbm, oc_v, in_sem.at[2]),
        pltpu.make_async_copy(vc_hbm, cots.at[0], in_sem.at[3]),
        pltpu.make_async_copy(gc_hbm, cots.at[1], in_sem.at[4]),
        pltpu.make_async_copy(co_hbm, cots.at[2], in_sem.at[5]),
        pltpu.make_async_copy(w0_hbm, wts[0], in_sem.at[6]),
        pltpu.make_async_copy(w1_hbm, wts[1], in_sem.at[7]),
        pltpu.make_async_copy(w2_hbm, wts[2], in_sem.at[8]),
    ]
    for load in loads:
        load.start()

    barrier = pltpu.get_barrier_semaphore()
    peers = [{"fs": lax.rem(z + k, nz) * nx + x} for k in range(1, nz)]
    peers += [{"fs": z * nx + lax.rem(x + k, nx)} for k in range(1, nx)]
    peers += [{"tp": lax.rem(t + k, tp)} for k in range(1, tp)]
    for peer in peers:
        pl.semaphore_signal(barrier, inc=1, device_id=peer, device_id_type=MESH)
    pl.semaphore_wait(barrier, len(peers))

    def stage_items(s, z_first):
        n1, n2 = (nz, nx) if z_first else (nx, nz)
        c1, c2 = (z, x) if z_first else (x, z)
        items = []
        for e in range(0, n2):
            d = s - e
            if d < 0 or d >= n1:
                continue
            for o1, s1, v1 in others(c1, n1, d):
                for o2, s2, v2 in others(c2, n2, e):
                    slot = o1 * nx + o2 if z_first else o2 * nx + o1
                    items.append((d, e, s1, s2, slot, both(v1, v2)))
        return items

    def forward(item, z_first, src, dst, ssem, rsem):
        d, e, s1, s2, slot, valid = item
        n1, n2 = (nz, nx) if z_first else (nx, nz)
        c1, c2 = (z, x) if z_first else (x, z)
        st1, st2 = (nx, 1) if z_first else (1, nx)
        if e == 0:
            if s1 in (-1, 0):
                send(src, dst, ssem(0), rsem, {"fs": me + st1}, c1 + 1 < n1, valid)
            if s1 in (1, 0):
                send(src, dst, ssem(1 if s1 == 0 else 0), rsem, {"fs": me - st1}, c1 > 0, valid)
        if s2 in (-1, 0):
            send(src, dst, ssem(2), rsem, {"fs": me + st2}, c2 + 1 < n2, valid)
        if s2 in (1, 0):
            send(src, dst, ssem(3 if s2 == 0 else 2), rsem, {"fs": me - st2}, c2 > 0, valid)

    def arrived(dst, sem, pred=None):
        run_if(pred, pltpu.make_async_copy(dst, dst, sem).wait)

    unit = block // 16
    half = core * (block // 2)
    fs_start = pl.multiple_of(half + row * 3 * unit, unit)
    y_send_start = pl.multiple_of(half + row * 5 * unit, unit)
    y_recv_start = pl.multiple_of(half + (1 - row) * 5 * unit, unit)
    mate_half = (1 - core) * (block // 2)
    mate_fs_start = pl.multiple_of(mate_half + row * 3 * unit, unit)
    mate_y_start = pl.multiple_of(mate_half + (1 - row) * 5 * unit, unit)

    def f_part(slot, start, units):
        return fg.at[slot, :, pl.ds(start, units * unit), :]

    def matmuls(slot, first):
        cols = pl.ds(pl.multiple_of(slot * block, block), block)
        tile = 256

        def body(i, carry):
            r = pl.ds(pl.multiple_of(i * tile, tile), tile)
            for k, src in enumerate((x_v, x_v, oc_v)):
                prod = jnp.dot(src[r, cols], fg[slot, k], preferred_element_type=F32)
                if first:
                    acc[k, r, :] = prod
                else:
                    acc[k, r, :] += prod
            return carry

        lax.fori_loop(0, tokens // tile, body, 0)

    n_stages = nz + nx - 1
    queued = {}
    for s in range(n_stages + 2):
        if s < n_stages:
            items = stage_items(s, True)
            queued[s] = items
            if s == 0:
                loads[0].wait()
            for item in items:
                d, e, s1, s2, slot, valid = item

                piece = f_part(slot, fs_start, 5)
                if s > 0:
                    arrived(piece, f_recv.at[slot], valid)
                forward(item, True, piece, piece, lambda i: f_send.at[slot, i], f_recv.at[slot])
                if s > 0:
                    ypiece = f_part(slot, y_send_start, 3)
                    send(ypiece, ypiece, y_send.at[slot], y_recv.at[slot], {"tp": beside}, None, valid)
                    send(piece, piece, p_send.at[slot, 0], p_recv.at[slot, 0], {"tp": mate}, None, valid)
        if s == 0:
            loads[1].wait()
            loads[2].wait()
            matmuls(me, True)
        if s - 1 >= 1 and s - 1 < n_stages:
            for item in queued[s - 1]:
                slot, valid = item[4], item[5]

                ypiece = f_part(slot, y_recv_start, 3)
                arrived(ypiece, y_recv.at[slot], valid)
                send(ypiece, ypiece, p_send.at[slot, 1], p_recv.at[slot, 1], {"tp": mate}, None, valid)
        if s - 2 >= 1:
            for item in queued[s - 2]:
                slot, valid = item[4], item[5]

                def use(slot=slot):
                    arrived(f_part(slot, mate_fs_start, 5), p_recv.at[slot, 0])
                    arrived(f_part(slot, mate_y_start, 3), p_recv.at[slot, 1])
                    matmuls(slot, False)

                run_if(valid, use)
    drain()

    for load in loads[3:6]:
        load.wait()
    dims = (((0,), (0,)), ((), ()))
    for k in range(3):
        upper, lower = high_low(acc[k])
        prod = lax.dot_general(upper, cots[k], dims, preferred_element_type=F32)
        prod = prod + lax.dot_general(lower, cots[k], dims, preferred_element_type=F32)
        part[:, k] = prod.reshape(n, rows, width)

    order = list(range(1, nz)) + [0]
    for k in order:
        oz = lax.rem(z + k, nz)
        for e in range(1, nx):
            ox = lax.rem(x + e, nx)
            send(
                part.at[oz * nx + ox], rx.at[e - 1, k], rx_send.at[e - 1, k], rx_recv.at[e - 1, k],
                {"fs": z * nx + ox}, None, None,
            )
    for k in order:
        oz = lax.rem(z + k, nz)
        value = part[oz * nx + x]
        for e in range(1, nx):
            arrived(rx.at[e - 1, k], rx_recv.at[e - 1, k])
            value = value + rx[e - 1, k]
        q[k] = value
        if k:
            send(q.at[k], rz.at[k - 1], rz_send.at[k - 1], rz_recv.at[k - 1], {"fs": oz * nx + x}, None, None)
    projected = q[0]
    for k in range(1, nz):
        arrived(rz.at[k - 1], rz_recv.at[k - 1])
        projected = projected + rz[k - 1]
    new_first = FIRST_DECAY * m1_ref[...] + (1.0 - FIRST_DECAY) * projected
    new_second = SECOND_DECAY * m2_ref[...] + (1.0 - SECOND_DECAY) * projected * projected
    nf_ref[...] = new_first
    ns_ref[...] = new_second
    dg[me] = new_first / (jnp.sqrt(new_second) + DIVISOR_EPS)

    for s in range(n_stages):
        for item in stage_items(s, True):
            slot, valid = item[4], item[5]
            piece = dg.at[slot]
            if s > 0:
                arrived(piece, d_recv.at[slot], valid)
            forward(item, True, piece, piece, lambda i: d_send.at[slot, i], d_recv.at[slot])

    total = jnp.zeros((1, width), F32)
    for i in range(n):
        for k in range(3):
            piece = dg[i, k]
            total = total + jnp.sum(piece * piece, axis=0, keepdims=True)
            upper, lower = high_low(piece)
            dh[k, i * rows:(i + 1) * rows, :] = upper
            dl[k, i * rows:(i + 1) * rows, :] = lower
    total = jnp.sum(total, axis=1, keepdims=True)
    ss[0] = jnp.broadcast_to(total, ss.shape[1:])
    for j in range(1, tp):
        send(ss.at[0], ss.at[j], s_send.at[j - 1], s_recv.at[j - 1], {"tp": lax.rem(t + j, tp)}, None, None)
    for load in loads[6:9]:
        load.wait()
    upd[0] = jnp.dot(fg[me, 0], dh[0], preferred_element_type=F32) + jnp.dot(
        fg[me, 0], dl[0], preferred_element_type=F32
    )
    upd[1] = jnp.dot(fg[me, 1], dh[1], preferred_element_type=F32) + jnp.dot(
        fg[me, 1], dl[1], preferred_element_type=F32
    )
    tdims = (((0,), (1,)), ((), ()))
    upd_t[...] = lax.dot_general(dh[2], fg[me, 2], tdims, preferred_element_type=F32) + lax.dot_general(
        dl[2], fg[me, 2], tdims, preferred_element_type=F32
    )
    sums = ss[0]
    for j in range(1, tp):
        arrived(ss.at[j], s_recv.at[j - 1])
        sums = sums + ss[j]
    scale = lax.rsqrt(sums[0:1, 0:1] / (3 * rank * width * tp) + SQUARE_EPS)

    outs = (c0_hbm, c1_hbm, c2_hbm)
    owns = (own01.at[0], own01.at[1], own2)
    news = (upd.at[0], upd.at[1], upd_t)
    upd_out = (u0_hbm, u1_hbm, u2_hbm)
    chunks = [(m, h) for m in range(3) for h in range(2)]

    def place(m, h, slot):
        if m < 2:
            size = block // 2
            return outs[m].at[pl.ds(pl.multiple_of(slot * block + h * size, size), size), :]
        size = width // 2
        return outs[m].at[pl.ds(h * size, size), pl.ds(pl.multiple_of(slot * block, block), block)]

    local = []
    for s in range(n_stages):
        for c, (m, h) in enumerate(chunks):
            z_first = c > 0
            if s == 0:
                size = (block if m < 2 else width) // 2
                r = pl.ds(h * size, size)
                update = scale * news[m][r, :]
                news[m][r, :] = update
                owns[m][r, :] = (wts[m][r, :] - LEARN_RATE * update).astype(BF16)
            for item in stage_items(s, z_first):
                slot, valid = item[4], item[5]
                dst = place(m, h, slot)
                src = dst
                if s > 0:
                    arrived(dst, c_recv.at[c, slot], valid)
                else:
                    size = (block if m < 2 else width) // 2
                    src = owns[m].at[pl.ds(h * size, size), :]
                forward(item, z_first, src, dst, lambda i: c_send.at[c, slot, i], c_recv.at[c, slot])
            if s == 0:
                size = (block if m < 2 else width) // 2
                r = pl.ds(h * size, size)
                local.append(pltpu.make_async_copy(owns[m].at[r, :], place(m, h, me), loc_sem.at[c]))
                local[-1].start()
                local.append(pltpu.make_async_copy(news[m].at[r, :], upd_out[m].at[r, :], loc_sem.at[6 + c]))
                local[-1].start()
    for copy in local:
        copy.wait()
    drain()


def shards(nz, nx, tp, *args):
    inputs, value_cot, gate_cot, out_cot, conv_output, factors, vw, gw, ow, m1, m2 = args
    n = nz * nx
    block, rank = factors.shape[1], factors.shape[2]
    rows, width = m1.shape[1], m1.shape[2]
    tokens = inputs.shape[0]
    features = inputs.shape[1]
    any_ = pl.BlockSpec(memory_space=pl.ANY)
    vmem = pl.BlockSpec(memory_space=pltpu.VMEM)
    dma = pltpu.SemaphoreType.DMA
    scratch = [
        pltpu.VMEM(inputs.shape, BF16),
        pltpu.VMEM(out_cot.shape, BF16),
        pltpu.VMEM((3, tokens, width), BF16),
        pltpu.VMEM((n, 3, block, rank), BF16),
        (pltpu.VMEM(vw.shape, F32), pltpu.VMEM(gw.shape, F32), pltpu.VMEM(ow.shape, F32)),
        pltpu.VMEM((3, tokens, rank), F32),
        pltpu.VMEM((n, 3, rows, width), F32),
        pltpu.VMEM((nx - 1, nz, 3, rows, width), F32),
        pltpu.VMEM((nz - 1, 3, rows, width), F32),
        pltpu.VMEM((nz, 3, rows, width), F32),
        pltpu.VMEM((n, 3, rows, width), F32),
        pltpu.VMEM((3, rank, width), BF16),
        pltpu.VMEM((3, rank, width), BF16),
        pltpu.VMEM((2, block, width), F32),
        pltpu.VMEM((width, block), F32),
        pltpu.VMEM((2, block, width), BF16),
        pltpu.VMEM((width, block), BF16),
        pltpu.VMEM((tp, 8, 128), F32),
        dma((9,)), dma((12,)),
        dma((n,)), dma((n, 4)), dma((n,)), dma((n,)), dma((n, 2)), dma((n, 2)),
        dma((nx - 1, nz)), dma((nx - 1, nz)), dma((nz - 1,)), dma((nz - 1,)),
        dma((n,)), dma((n, 4)), dma((tp - 1,)), dma((tp - 1,)),
        dma((6, n)), dma((6, n, 4)),
    ]
    shape = jax.ShapeDtypeStruct
    return pl.pallas_call(
        functools.partial(kernel, nz, nx, tp),
        out_shape=(
            shape(m1.shape, F32), shape(m2.shape, F32),
            shape(vw.shape, F32), shape(gw.shape, F32), shape(ow.shape, F32),
            shape((features, width), BF16), shape((features, width), BF16), shape((width, features), BF16),
        ),
        in_specs=[any_] * 9 + [vmem] * 2,
        out_specs=(vmem, vmem) + (any_,) * 6,
        scratch_shapes=scratch,
        compiler_params=pltpu.CompilerParams(
            collective_id=0, has_side_effects=True, vmem_limit_bytes=60 * 1024 * 1024
        ),
    )(inputs, out_cot, value_cot, gate_cot, conv_output, factors, vw, gw, ow, m1, m2)


def solution(mesh):
    fs, tp = mesh.shape["fs"], mesh.shape["tp"]
    nz = 1 << (fs.bit_length() // 2)
    nx = fs // nz
    placed = (
        P("fs", None),
        P("fs", "tp"),
        P("fs", "tp"),
        P("fs", None),
        P("fs", "tp"),
        P(None, "fs", None),
        P("fs", "tp"),
        P("fs", "tp"),
        P("tp", "fs"),
        P(None, "fs", "tp"),
        P(None, "fs", "tp"),
    )
    return jax.shard_map(
        functools.partial(shards, nz, nx, tp),
        mesh=mesh,
        in_specs=placed,
        out_specs=(
            P(None, "fs", "tp"),
            P(None, "fs", "tp"),
            P("fs", "tp"),
            P("fs", "tp"),
            P("tp", "fs"),
            P(None, "tp"),
            P(None, "tp"),
            P("tp", None),
        ),
        check_vma=False,
    )
```

```python
import functools

import jax
import jax.numpy as jnp
from jax import lax
from jax.experimental import pallas as pl
from jax.experimental.pallas import tpu as pltpu
from jax.sharding import PartitionSpec as P

FIRST_DECAY = 0.9
SECOND_DECAY = 0.95
DIVISOR_EPS = 1e-08
SQUARE_EPS = 1e-06
LEARN_RATE = 0.01
HOP, SKEW, SKEW2, RS_X, RS_Z, HOP_D = 4.2, 1.8, 3.0, 8.0, 6.0, 3.7
VMEM_BYTES = 45 * 1024 * 1024
MESH = pl.DeviceIdType.MESH
F32 = jnp.float32
BF16 = jnp.bfloat16


def high_low(values):
    upper = values.astype(BF16)
    lower = (values - upper.astype(F32)).astype(BF16)
    return upper, lower


def others(coord, size, dist):
    if dist == 0:
        return [(coord, 0, None)]
    if size == 2:
        return [(1 - coord, None, None)]
    return [(coord - dist, -1, coord >= dist), (coord + dist, 1, coord + dist < size)]


def both(*preds):
    preds = [p for p in preds if p is not None]
    if not preds:
        return None
    return functools.reduce(jnp.logical_and, preds)


def run_if(pred, fn):
    if pred is None:
        fn()
    else:
        pl.when(pred)(fn)


def kernel(
    nz, nx, tp,
    x_hbm, oc_hbm, vc_hbm, gc_hbm, co_hbm, f_hbm, w0_hbm, w1_hbm, w2_hbm, m1_ref, m2_ref,
    nf_ref, ns_ref, u0_ref, u1_ref, u2_ref, c0_ref, c1_ref, c2_ref,
    x_v, oc_v, cots, fg, wts, acc, part, rx, rz, q, dg, dh, dl, ss,
    in_sem, f_recv, f_send, y_recv, y_send, p_recv, p_send,
    rx_recv, rx_send, rz_recv, rz_send, d_recv, d_send, s_recv, s_send, c_recv, c_send,
):
    me = lax.axis_index("fs")
    t = lax.axis_index("tp")
    z = lax.div(me, nx)
    x = lax.rem(me, nx)
    n = nz * nx
    core = lax.rem(t, 2)
    row = lax.rem(lax.div(t, 2), 2)
    mate = t + 1 - 2 * core
    beside = t + 2 - 4 * row
    block = f_hbm.shape[1]
    rank = f_hbm.shape[2]
    rows = m1_ref.shape[1]
    width = m1_ref.shape[2]
    tokens = x_hbm.shape[0]
    pending = []

    def remote(src, dst, ssem, rsem, where):
        copy = pltpu.make_async_remote_copy(
            src_ref=src, dst_ref=dst, send_sem=ssem, recv_sem=rsem,
            device_id=where, device_id_type=MESH,
        )
        return copy

    def send(src, dst, ssem, rsem, where, pred, outer):
        copy = remote(src, dst, ssem, rsem, where)
        pred = both(pred, outer)
        run_if(pred, copy.start)
        pending.append((pred, copy))

    def drain():
        for pred, copy in pending:
            run_if(pred, copy.wait_send)
        pending.clear()

    loads = [
        pltpu.make_async_copy(f_hbm, fg.at[:, me], in_sem.at[0]),
        pltpu.make_async_copy(x_hbm, x_v, in_sem.at[1]),
        pltpu.make_async_copy(oc_hbm, oc_v, in_sem.at[2]),
        pltpu.make_async_copy(vc_hbm, cots.at[0], in_sem.at[3]),
        pltpu.make_async_copy(gc_hbm, cots.at[1], in_sem.at[4]),
        pltpu.make_async_copy(co_hbm, cots.at[2], in_sem.at[5]),
        pltpu.make_async_copy(w0_hbm, wts[0], in_sem.at[6]),
        pltpu.make_async_copy(w1_hbm, wts[1], in_sem.at[7]),
        pltpu.make_async_copy(w2_hbm, wts[2], in_sem.at[8]),
    ]
    for load in loads:
        load.start()

    barrier = pltpu.get_barrier_semaphore()
    peers = [{"fs": lax.rem(z + k, nz) * nx + x} for k in range(1, nz)]
    peers += [{"fs": z * nx + lax.rem(x + k, nx)} for k in range(1, nx)]
    peers += [{"tp": lax.rem(t + k, tp)} for k in range(1, tp)]
    for peer in peers:
        pl.semaphore_signal(barrier, inc=1, device_id=peer, device_id_type=MESH)
    pl.semaphore_wait(barrier, len(peers))

    def stage_items(s, z_first):
        n1, n2 = (nz, nx) if z_first else (nx, nz)
        c1, c2 = (z, x) if z_first else (x, z)
        items = []
        for e in range(0, n2):
            d = s - e
            if d < 0 or d >= n1:
                continue
            for o1, s1, v1 in others(c1, n1, d):
                for o2, s2, v2 in others(c2, n2, e):
                    slot = o1 * nx + o2 if z_first else o2 * nx + o1
                    items.append((d, e, s1, s2, slot, both(v1, v2)))
        return items

    def forward(item, z_first, src, dst, ssem, rsem):
        d, e, s1, s2, slot, valid = item
        n1, n2 = (nz, nx) if z_first else (nx, nz)
        c1, c2 = (z, x) if z_first else (x, z)
        st1, st2 = (nx, 1) if z_first else (1, nx)
        if e == 0:
            if s1 in (-1, 0):
                send(src, dst, ssem(0), rsem, {"fs": me + st1}, c1 + 1 < n1, valid)
            if s1 in (1, 0):
                send(src, dst, ssem(1 if s1 == 0 else 0), rsem, {"fs": me - st1}, c1 > 0, valid)
        if s2 in (-1, 0):
            send(src, dst, ssem(2), rsem, {"fs": me + st2}, c2 + 1 < n2, valid)
        if s2 in (1, 0):
            send(src, dst, ssem(3 if s2 == 0 else 2), rsem, {"fs": me - st2}, c2 > 0, valid)

    def arrived(dst, sem, pred=None):
        run_if(pred, pltpu.make_async_copy(dst, dst, sem).wait)

    unit = block // 16
    half = core * (block // 2)
    fs_start = pl.multiple_of(half + row * 3 * unit, unit)
    y_send_start = pl.multiple_of(half + row * 5 * unit, unit)
    y_recv_start = pl.multiple_of(half + (1 - row) * 5 * unit, unit)
    mate_half = (1 - core) * (block // 2)
    mate_fs_start = pl.multiple_of(mate_half + row * 3 * unit, unit)
    mate_y_start = pl.multiple_of(mate_half + (1 - row) * 5 * unit, unit)

    def f_part(k, slot, start, units):
        return fg.at[k, slot, pl.ds(start, units * unit), :]

    sources = (x_v, x_v, oc_v)

    def matmul(k, slot, first):
        cols = pl.ds(pl.multiple_of(slot * block, block), block)
        tile = 256

        def body(i, carry):
            r = pl.ds(pl.multiple_of(i * tile, tile), tile)
            prod = jnp.dot(sources[k][r, cols], fg[k, slot], preferred_element_type=F32)
            if first:
                acc[k, r, :] = prod
            else:
                acc[k, r, :] += prod
            return carry

        lax.fori_loop(0, tokens // tile, body, 0)

    n_stages = nz + nx - 1
    stages = [stage_items(s, True) for s in range(n_stages)]

    def f_arrive(k, s):
        for item in stages[s]:
            slot, valid = item[4], item[5]
            piece = f_part(k, slot, fs_start, 5)
            if s > 0:
                arrived(piece, f_recv.at[k, slot], valid)
            forward(item, True, piece, piece, lambda i: f_send.at[k, slot, i], f_recv.at[k, slot])
            if s > 0:
                ypiece = f_part(k, slot, y_send_start, 3)
                send(ypiece, ypiece, y_send.at[k, slot], y_recv.at[k, slot], {"tp": beside}, None, valid)
                send(piece, piece, p_send.at[k, slot, 0], p_recv.at[k, slot, 0], {"tp": mate}, None, valid)

    def f_pass(k, s):
        for item in stages[s]:
            slot, valid = item[4], item[5]
            ypiece = f_part(k, slot, y_recv_start, 3)
            arrived(ypiece, y_recv.at[k, slot], valid)
            send(ypiece, ypiece, p_send.at[k, slot, 1], p_recv.at[k, slot, 1], {"tp": mate}, None, valid)

    def f_use(k, s):
        for item in stages[s]:
            slot, valid = item[4], item[5]

            def use(slot=slot):
                arrived(f_part(k, slot, mate_fs_start, 5), p_recv.at[k, slot, 0])
                arrived(f_part(k, slot, mate_y_start, 3), p_recv.at[k, slot, 1])
                matmul(k, slot, False)

            run_if(valid, use)

    dims = (((0,), (0,)), ((), ()))
    order = list(range(1, nz)) + [0]

    def partial(k):
        loads[3 + k].wait()
        upper, lower = high_low(acc[k])
        prod = lax.dot_general(upper, cots[k], dims, preferred_element_type=F32)
        prod = prod + lax.dot_general(lower, cots[k], dims, preferred_element_type=F32)
        part[k] = prod.reshape(n, rows, width)
        for i in order:
            oz = lax.rem(z + i, nz)
            for e in range(1, nx):
                slot = oz * nx + lax.rem(x + e, nx)
                send(
                    part.at[k, slot], rx.at[k, e - 1, i], rx_send.at[k, e - 1, i], rx_recv.at[k, e - 1, i],
                    {"fs": z * nx + lax.rem(x + e, nx)}, None, None,
                )

    def along_z(k):
        for i in order:
            oz = lax.rem(z + i, nz)
            value = part[k, oz * nx + x]
            for e in range(1, nx):
                arrived(rx.at[k, e - 1, i], rx_recv.at[k, e - 1, i])
                value = value + rx[k, e - 1, i]
            q[k, i] = value
            if i:
                send(
                    q.at[k, i], rz.at[k, i - 1], rz_send.at[k, i - 1], rz_recv.at[k, i - 1],
                    {"fs": oz * nx + x}, None, None,
                )

    def moments(k):
        projected = q[k, 0]
        for i in range(1, nz):
            arrived(rz.at[k, i - 1], rz_recv.at[k, i - 1])
            projected = projected + rz[k, i - 1]
        new_first = FIRST_DECAY * m1_ref[k] + (1.0 - FIRST_DECAY) * projected
        new_second = SECOND_DECAY * m2_ref[k] + (1.0 - SECOND_DECAY) * projected * projected
        nf_ref[k] = new_first
        ns_ref[k] = new_second
        dg[k, me] = new_first / (jnp.sqrt(new_second) + DIVISOR_EPS)
        d_arrive(k, 0)

    def d_arrive(k, s):
        for item in stages[s]:
            slot, valid = item[4], item[5]
            piece = dg.at[k, slot]
            if s > 0:
                arrived(piece, d_recv.at[k, slot], valid)
            forward(item, True, piece, piece, lambda i: d_send.at[k, slot, i], d_recv.at[k, slot])

    tdims = (((0,), (1,)), ((), ()))
    news = (u0_ref, u1_ref, u2_ref)

    def unscaled(k):
        value = dg[k].reshape(rank, width)
        upper, lower = high_low(value)
        dh[k] = upper
        dl[k] = lower
        if k < 2:
            news[k][...] = jnp.dot(fg[k, me], dh[k], preferred_element_type=F32) + jnp.dot(
                fg[k, me], dl[k], preferred_element_type=F32
            )
        else:
            news[k][...] = lax.dot_general(dh[k], fg[k, me], tdims, preferred_element_type=F32) + lax.dot_general(
                dl[k], fg[k, me], tdims, preferred_element_type=F32
            )

    def squares(k):
        value = dg[k].reshape(rank, width)
        return jnp.sum(value * value, axis=0, keepdims=True)

    loads[0].wait()
    for k in range(3):
        f_arrive(k, 0)

    def own_part(k):
        if k != 1:
            loads[1 + k // 2].wait()
        matmul(k, me, True)

    steps = []
    hop, skew = HOP, SKEW
    for k in range(3):
        for s in range(1, n_stages):
            at = s * hop + k * skew
            steps.append((at, 0, k, s, f_arrive))
            steps.append((at + 3.5, 1, k, s, f_pass))
            steps.append((at + 6.0, 2, k, s, f_use))
        steps.append((8.5 + 0.5 * k, 2, k, None, own_part))
        at = (n_stages - 1) * hop + 8.0 + k * SKEW2
        steps.append((at, 3, k, None, partial))
        steps.append((at + RS_X, 4, k, None, along_z))
        at = at + RS_X + RS_Z
        steps.append((at, 5, k, None, moments))
        for s in range(1, n_stages):
            steps.append((at + s * HOP_D, 6, k, s, d_arrive))
    steps.sort(key=lambda step: step[:3])
    for _, _, k, s, step in steps:
        if s is None:
            step(k)
        else:
            step(k, s)
    unscaled(0)
    total = squares(0)
    total = jnp.sum(total + squares(1) + squares(2), axis=1, keepdims=True)
    ss[0] = jnp.broadcast_to(total, ss.shape[1:])
    for j in range(1, tp):
        send(ss.at[0], ss.at[j], s_send.at[j - 1], s_recv.at[j - 1], {"tp": lax.rem(t + j, tp)}, None, None)
    unscaled(1)
    unscaled(2)
    for load in loads[6:9]:
        load.wait()
    sums = ss[0]
    for j in range(1, tp):
        arrived(ss.at[j], s_recv.at[j - 1])
        sums = sums + ss[j]
    scale = lax.rsqrt(sums[0:1, 0:1] / (3 * rank * width * tp) + SQUARE_EPS)

    outs = (c0_ref, c1_ref, c2_ref)
    chunks = [(m, h) for m in range(3) for h in range(2)]

    def place(m, h, slot):
        if m < 2:
            size = block // 2
            return outs[m].at[pl.ds(pl.multiple_of(slot * block + h * size, size), size), :]
        size = width // 2
        return outs[m].at[pl.ds(h * size, size), pl.ds(pl.multiple_of(slot * block, block), block)]

    for s in range(n_stages):
        for c, (m, h) in enumerate(chunks):
            z_first = c > 0
            if s == 0:
                size = (block if m < 2 else width) // 2
                r = pl.ds(h * size, size)
                update = scale * news[m][r, :]
                news[m][r, :] = update
                place(m, h, me)[...] = (wts[m][r, :] - LEARN_RATE * update).astype(BF16)
            for item in stage_items(s, z_first):
                slot, valid = item[4], item[5]
                dst = place(m, h, slot)
                if s > 0:
                    arrived(dst, c_recv.at[c, slot], valid)
                forward(item, z_first, dst, dst, lambda i: c_send.at[c, slot, i], c_recv.at[c, slot])
    drain()


def store_kernel(*refs):
    count = (len(refs) - 1) // 2
    sems = refs[-1]
    copies = [pltpu.make_async_copy(refs[i], refs[count + i], sems.at[i]) for i in range(count)]
    for copy in copies:
        copy.start()
    for copy in copies:
        copy.wait()


def shards(nz, nx, tp, *args):
    inputs, value_cot, gate_cot, out_cot, conv_output, factors, vw, gw, ow, m1, m2 = args
    n = nz * nx
    block, rank = factors.shape[1], factors.shape[2]
    rows, width = m1.shape[1], m1.shape[2]
    tokens = inputs.shape[0]
    features = inputs.shape[1]
    any_ = pl.BlockSpec(memory_space=pl.ANY)
    vmem = pl.BlockSpec(memory_space=pltpu.VMEM)
    dma = pltpu.SemaphoreType.DMA
    scratch = [
        pltpu.VMEM(inputs.shape, BF16),
        pltpu.VMEM(out_cot.shape, BF16),
        pltpu.VMEM((3, tokens, width), BF16),
        pltpu.VMEM((3, n, block, rank), BF16),
        (pltpu.VMEM(vw.shape, F32), pltpu.VMEM(gw.shape, F32), pltpu.VMEM(ow.shape, F32)),
        pltpu.VMEM((3, tokens, rank), F32),
        pltpu.VMEM((3, n, rows, width), F32),
        pltpu.VMEM((3, nx - 1, nz, rows, width), F32),
        pltpu.VMEM((3, nz - 1, rows, width), F32),
        pltpu.VMEM((3, nz, rows, width), F32),
        pltpu.VMEM((3, n, rows, width), F32),
        pltpu.VMEM((3, rank, width), BF16),
        pltpu.VMEM((3, rank, width), BF16),
        pltpu.VMEM((tp, 8, 128), F32),
        dma((9,)),
        dma((3, n)), dma((3, n, 4)), dma((3, n)), dma((3, n)), dma((3, n, 2)), dma((3, n, 2)),
        dma((3, nx - 1, nz)), dma((3, nx - 1, nz)), dma((3, nz - 1)), dma((3, nz - 1)),
        dma((3, n)), dma((3, n, 4)), dma((tp - 1,)), dma((tp - 1,)),
        dma((6, n)), dma((6, n, 4)),
    ]
    shape = [
        (m1.shape, F32), (m2.shape, F32), (vw.shape, F32), (gw.shape, F32), (ow.shape, F32),
        ((features, width), BF16), ((features, width), BF16), ((width, features), BF16),
    ]
    held = pl.pallas_call(
        functools.partial(kernel, nz, nx, tp),
        out_shape=tuple(pltpu.VMEM(*item) for item in shape),
        in_specs=[any_] * 9 + [vmem] * 2,
        out_specs=(vmem,) * 8,
        scratch_shapes=scratch,
        compiler_params=pltpu.CompilerParams(
            collective_id=0, has_side_effects=True, vmem_limit_bytes=VMEM_BYTES
        ),
    )(inputs, out_cot, value_cot, gate_cot, conv_output, factors, vw, gw, ow, m1, m2)
    return pl.pallas_call(
        store_kernel,
        out_shape=tuple(jax.ShapeDtypeStruct(*item) for item in shape),
        in_specs=[vmem] * 8,
        out_specs=(any_,) * 8,
        scratch_shapes=[dma((8,))],
        compiler_params=pltpu.CompilerParams(vmem_limit_bytes=1024 * 1024),
    )(*held)


def solution(mesh):
    fs, tp = mesh.shape["fs"], mesh.shape["tp"]
    nz = 1 << (fs.bit_length() // 2)
    nx = fs // nz
    placed = (
        P("fs", None),
        P("fs", "tp"),
        P("fs", "tp"),
        P("fs", None),
        P("fs", "tp"),
        P(None, "fs", None),
        P("fs", "tp"),
        P("fs", "tp"),
        P("tp", "fs"),
        P(None, "fs", "tp"),
        P(None, "fs", "tp"),
    )
    return jax.shard_map(
        functools.partial(shards, nz, nx, tp),
        mesh=mesh,
        in_specs=placed,
        out_specs=(
            P(None, "fs", "tp"),
            P(None, "fs", "tp"),
            P("fs", "tp"),
            P("fs", "tp"),
            P("tp", "fs"),
            P(None, "tp"),
            P(None, "tp"),
            P("tp", None),
        ),
        check_vma=False,
    )
```
